256 devices in a mesh: sp: 64 (over z, x, core), tp: 4 (over y).
Axes of the slice: x: 4, y: 4, z: 8, core: 2. Of those that a mesh axis runs over, the one named last changes fastest.
Arguments:
- layer_input: bfloat16 [8192, 2048], P('sp'), may hold values from -6 to 6
- out_cot: bfloat16 [8192, 2048], P('sp'), may hold values from -16 to 16
- routes: int32 [8192, 2], P('sp'), may hold values from 0 to 63, all different within a row; in each aligned block of 128 rows (0 to 127, 128 to 255, ...) at most 8 rows name the same one
- route_weights: float32 [8192, 2], P('sp'), may hold values from 0.2 to 1
- gate_weights: bfloat16 [64, 2048, 1024], P('sp', None, 'tp'), may hold values from -0.125 to 0.125
- up_weights: bfloat16 [64, 2048, 1024], P('sp', None, 'tp'), may hold values from -0.125 to 0.125
- down_weights: bfloat16 [64, 1024, 2048], P('sp', 'tp'), may hold values from -0.1875 to 0.1875
- out_proj: bfloat16 [2048, 2048], P(None, 'tp'), may hold values from -0.125 to 0.125
- queries: bfloat16 [8192, 2048], P('sp', 'tp'), may hold values from -6 to 6
- keys: bfloat16 [8192, 2048], P('sp', 'tp'), may hold values from -6 to 6
- values: bfloat16 [8192, 2048], P('sp', 'tp'), may hold values from -6 to 6
- mixer_out: bfloat16 [8192, 2048], P('sp', 'tp'), may hold values from -6 to 6
- entry_states: float32 [64, 32, 64, 64], P('sp', 'tp'), may hold values from -6 to 6
Outputs:
- grad_gate: bfloat16 [64, 2048, 1024], P('sp', None, 'tp')
- grad_up: bfloat16 [64, 2048, 1024], P('sp', None, 'tp')
- grad_down: bfloat16 [64, 1024, 2048], P('sp', 'tp')
- grad_proj: float32 [2048, 2048], P('sp', 'tp')
- grad_queries: bfloat16 [8192, 2048], P('sp', 'tp')
- grad_keys: bfloat16 [8192, 2048], P('sp', 'tp')
- grad_values: bfloat16 [8192, 2048], P('sp', 'tp')
The draws below stay inside these ranges and needn't reach their ends.
Inputs may be any that keep to these rules, and one draw needn't show every extreme that they name: `routes`: in each aligned block of 128 rows no expert is named by more than 8 rows, a bound that some block reaches; the numbers of one row differ.
All inputs are finite; a program needn't handle non-finite values.
Results may differ from the reference program's by a relative error of at most 0.01.
Values may be sent and summed in bfloat16 or wider, within the bound.
A program may use at most 128 MiB of HBM per device.

```python
import math
import jax
import jax.numpy as jnp
import numpy as np
from jax import lax

D = 2048
FF = 1024
HEADS = 32
DK = 64
TOPK = 2
SPAN = 128
TOK_DEV = 128
TOKENS = 8192
EXPERTS = 64
CAP = 8
HV = 2048
N_SP = 64


def raised(array, stream_key, source, target, shards_of, factor):
    def block_of(dim):
        return (jnp.arange(array.shape[dim]) // (array.shape[dim] // shards_of)).reshape((-1,) + (1,) * (array.ndim - 1 - dim))

    near = jax.random.permutation(stream_key, shards_of)[block_of(target)]
    far = (block_of(target) + shards_of // 2) % shards_of
    return jnp.where((block_of(source) == near) | (block_of(source) == far), factor * array, array)


def block_levels(rng, extent, split, smallest, high):
    level, own = 1.0, jax.random.fold_in(rng, 6)
    for axis_at, parts in split:
        heights = jnp.exp(jax.random.uniform(jax.random.fold_in(own, axis_at), (parts,), jnp.float32, smallest / len(split), high / len(split)))
        level = level * jnp.repeat(heights, extent[axis_at] // parts).reshape([-1 if axis == axis_at else 1 for axis in range(len(extent))])
    return level


def routed_block(rng, own, number, rows, amount, top, limit, lean):
    sequence = jax.random.permutation(rng, amount)
    heavy_load, common = shares(amount, rows * top, limit, lean, True), shares(amount, rows * top, limit, lean, False)
    places = jnp.arange(amount)

    def named(tallies, turn):
        used = int((tallies > 0).sum())
        fixed = max(1, used // 4)
        moved = fixed + (places - fixed + turn * (used - fixed)) % max(1, amount - fixed)
        return jnp.zeros((amount,), jnp.int32).at[sequence[jnp.where(places < fixed, places, moved)]].set(jnp.asarray(tallies, jnp.int32))

    tallies = jnp.where(number % 4 == 0, named(heavy_load, number // 4), named(common, number - number // 4 - 1))
    mixed = jax.random.permutation(jax.random.fold_in(own, 3), amount)
    donor, receiver = mixed[0:amount // 2 * 2:2], mixed[1:amount // 2 * 2:2]
    slack = jnp.minimum(tallies[donor] - 1, limit - tallies[receiver]) // 2
    slack = jnp.where((donor == sequence[0]) | (receiver == sequence[0]) | (tallies[receiver] == 0), 0, jnp.maximum(slack, 0))
    moved = jax.random.randint(jax.random.fold_in(own, 4), (amount // 2,), 0, 1 << 20) % (slack + 1)
    tallies = tallies.at[donor].add(-moved).at[receiver].add(moved)
    members = jnp.searchsorted(jnp.cumsum(tallies), jnp.arange(rows * top), side="right").astype(jnp.int32)
    listing = members.reshape(top, rows).T
    listing = listing[jax.random.permutation(jax.random.fold_in(own, 1), rows)]
    turn = jax.random.randint(jax.random.fold_in(own, 2), (rows, 1), 0, top)
    return jnp.take_along_axis(listing, (jnp.arange(top)[None, :] + turn) % top, axis=1)


def shares(number_of, total, bound, skew, full):
    weights = [(1 << 20) // math.isqrt(grade ** skew) + 1 for grade in range(1, number_of + 1)]
    largest = bound if full else min(bound, max(-(-total // number_of), total * weights[0] // sum(weights)))
    least = 1 if total - largest >= number_of - 1 else 0
    counts, surplus = [largest] + [least] * (number_of - 1), total - largest - least * (number_of - 1)
    while surplus > 0:
        candidates = [i for i in range(1, number_of) if counts[i] < largest] or [i for i in range(1, number_of) if counts[i] < bound]
        whole, left = sum([weights[i] for i in candidates]), surplus
        for i in candidates:
            more = min(bound - counts[i], max(1, left * weights[i] // whole), surplus)
            counts[i] = counts[i] + more
            surplus = surplus - more
    return np.array(counts)


def noise(rng, shape, spread, limit, pieces=(), kind=jnp.bfloat16):
    drawn = jax.random.normal(rng, shape, jnp.float32) * spread
    if len(pieces) > 0:
        drawn = block_levels(rng, shape, pieces, -0.22, 0.18) * drawn
    return jnp.clip(drawn, min=-limit, max=limit).astype(kind)


def bell_draw_with(key, shape, scale, limit, split, heavy, held_as=jnp.bfloat16):
    values = scale * jax.random.normal(key, shape, jnp.float32)
    if split:
        values = values * block_levels(key, shape, split, -0.22, 0.18)
    return jnp.clip(raised(values, jax.random.fold_in(key, 3), *heavy), -limit, limit).astype(held_as)


def setup_inputs(seed: int = 0) -> dict:
    seeds = jax.random.split(jax.random.key(seed), 14)
    layer_input = noise(seeds[0], (TOKENS, D), 1.0, 6.0, ((0, 64),))
    out_cot = bell_draw_with(seeds[1], (TOKENS, D), 1.0, 16.0, ((0, 64),), (0, 1, 64, 4.0))
    routes_keys = jax.random.split(jax.random.fold_in(seeds[2], 1), TOKENS // TOK_DEV)
    routes_turns = jax.random.permutation(jax.random.fold_in(seeds[2], 3), TOKENS // TOK_DEV)
    routes = jax.vmap(lambda own, number: routed_block(jax.random.fold_in(seeds[2], 2), own, number, TOK_DEV, EXPERTS, TOPK, CAP, 1))(routes_keys, routes_turns).reshape((TOKENS, TOPK))
    route_weights = jnp.clip(0.2 + 0.8 * jax.random.uniform(seeds[3], (TOKENS, TOPK), jnp.float32) ** block_levels(seeds[3], (TOKENS, TOPK), ((0, 64),), -0.2, 0.2), 0.2, 1.0)
    gate_weights = noise(seeds[4], (EXPERTS, D, FF), D ** -0.5, 0.125, ((0, 64), (2, 4)))
    up_weights = noise(seeds[5], (EXPERTS, D, FF), D ** -0.5, 0.125, ((0, 64), (2, 4)))
    down_weights = noise(seeds[6], (EXPERTS, FF, D), FF ** -0.5, 0.1875, ((0, 64), (1, 4)))
    out_proj = noise(seeds[7], (D, HV), HV ** -0.5, 0.125, ((1, 4),))
    queries = noise(seeds[8], (TOKENS, HV), 1.0, 6.0, ((0, 64), (1, 4)))
    keys = noise(seeds[9], (TOKENS, HV), 1.0, 6.0, ((0, 64), (1, 4)))
    values = noise(seeds[10], (TOKENS, HV), 1.0, 6.0, ((0, 64), (1, 4)))
    mixer_out = noise(seeds[11], (TOKENS, HV), 1.0, 6.0, ((0, 64), (1, 4)))
    entry_states = noise(seeds[12], (N_SP, HEADS, DK, DK), 1.0, 6.0, ((0, 64), (1, 4)), jnp.float32)
    return dict(layer_input=layer_input, out_cot=out_cot, routes=routes, route_weights=route_weights, gate_weights=gate_weights, up_weights=up_weights, down_weights=down_weights, out_proj=out_proj, queries=queries, keys=keys, values=values, mixer_out=mixer_out, entry_states=entry_states)


def decay_rates(head_ids, head_count, token_count):
    half_count = head_count // 2
    fraction = jnp.minimum(head_ids, half_count) / half_count
    base_rate = jnp.exp((1.0 - fraction) * jnp.log(1.0 / 32.0) + fraction * jnp.log(1.0 / token_count))
    return base_rate * (1.0 + jnp.maximum(head_ids - half_count, 0.0) / half_count)

def position_norm(positions, head_rates):
    return jnp.sqrt(jnp.expm1(-2.0 * head_rates)[None, :] / jnp.expm1(-2.0 * head_rates[None, :] * (positions[:, None] + 1.0)))

def rounded(values):
    return lax.optimization_barrier(values.astype(jnp.bfloat16)).astype(jnp.float32)

def retention_grads(queries, keys, values, head_cot, entry_states, head_rates):
    span_count = TOKENS // SPAN
    per_segment = TOK_DEV // SPAN
    key_scale = DK ** (-0.5)
    span_shape = (span_count, SPAN, HEADS, DK)
    query_wide = queries.reshape(span_shape).astype(jnp.float32)
    key_wide = keys.reshape(span_shape).astype(jnp.float32)
    value_wide = values.reshape(span_shape).astype(jnp.float32)
    cot_wide = head_cot.reshape(span_shape).astype(jnp.float32)
    offsets = jnp.arange(SPAN).astype(jnp.float32)
    distance = offsets[:, None] - offsets[None, :]
    decay_mat = jnp.where(distance[None] >= 0, jnp.exp(-head_rates[:, None, None] * jnp.maximum(distance, 0.0)[None]), 0.0)
    fwd_weights = rounded(jnp.einsum('cihd,cjhd->chij', query_wide, key_wide) * key_scale * decay_mat[None])
    back_weights = rounded(jnp.einsum('cihd,cjhd->chij', cot_wide, value_wide) * decay_mat[None])
    tail_decay = jnp.exp(-head_rates[None, :] * (SPAN - 1.0 - offsets)[:, None])
    lead_decay = jnp.exp(-head_rates[None, :] * (offsets + 1.0)[:, None])
    span_decay = jnp.exp(-head_rates * SPAN)
    updates = key_scale * jnp.einsum('cjhd,cjhe->chde', key_wide * tail_decay[None, :, :, None], value_wide, precision=lax.Precision.HIGHEST)
    backs = jnp.einsum('cihd,cihe->chde', query_wide * lead_decay[None, :, :, None], cot_wide, precision=lax.Precision.HIGHEST)

    def forward(carried, inputs_c):
        update, span_index = inputs_c
        saved_state = entry_states[span_index // per_segment]
        current = jnp.where(span_index % per_segment == 0, saved_state, carried)
        return (span_decay[:, None, None] * current + update, current)
    start_state = jnp.zeros((HEADS, DK, DK), jnp.float32)
    _, fwd_states = lax.scan(forward, start_state, (updates, jnp.arange(span_count, dtype=jnp.int32)))

    def backward(carried, update):
        return (span_decay[:, None, None] * carried + update, carried)
    _, rev_states = lax.scan(backward, start_state, backs, reverse=True)
    grad_q = key_scale * jnp.einsum('chij,cjhd->cihd', back_weights, key_wide)
    grad_q = grad_q + lead_decay[None, :, :, None] * jnp.einsum('chde,cihe->cihd', fwd_states, cot_wide, precision=lax.Precision.HIGHEST)
    grad_k = jnp.einsum('chij,cihd->cjhd', back_weights, query_wide)
    grad_k = key_scale * (grad_k + tail_decay[None, :, :, None] * jnp.einsum('chde,cjhe->cjhd', rev_states, value_wide, precision=lax.Precision.HIGHEST))
    grad_v = jnp.einsum('chij,cihe->cjhe', fwd_weights, cot_wide)
    grad_v = grad_v + key_scale * tail_decay[None, :, :, None] * jnp.einsum('chde,cjhd->cjhe', rev_states, key_wide, precision=lax.Precision.HIGHEST)
    flat_shape = (TOKENS, HEADS * DK)
    return (grad_q.reshape(flat_shape).astype(jnp.bfloat16), grad_k.reshape(flat_shape).astype(jnp.bfloat16), grad_v.reshape(flat_shape).astype(jnp.bfloat16))

def reference(layer_input, out_cot, routes, route_weights, gate_weights, up_weights, down_weights, out_proj, queries, keys, values, mixer_out, entry_states):
    pair_total = TOKENS * TOPK
    per_block = TOK_DEV * TOPK
    slot_count = N_SP * CAP
    flat_routes = routes.reshape(-1)
    onehot = (flat_routes.reshape(N_SP, per_block, 1) == jnp.arange(EXPERTS, dtype=jnp.int32)[None, None, :]).astype(jnp.int32)
    earlier = jnp.cumsum(onehot, axis=1) - onehot
    placed = lax.optimization_barrier(jnp.sum(earlier * onehot, axis=2)).reshape(-1)
    block_id = jnp.arange(pair_total, dtype=jnp.int32) // per_block
    target = flat_routes * slot_count + block_id * CAP + placed
    owner_tok = jnp.arange(pair_total, dtype=jnp.int32) // TOPK
    slot_tok = jnp.full((EXPERTS * slot_count,), TOKENS, jnp.int32).at[target].set(owner_tok)
    slot_weight = jnp.zeros((EXPERTS * slot_count,), jnp.float32).at[target].set(route_weights.reshape(-1))
    blank_row = jnp.zeros((1, D), jnp.bfloat16)
    input_ext = jnp.concatenate([layer_input, blank_row], 0)
    cot_ext = jnp.concatenate([out_cot, blank_row], 0)

    def expert_step(accum, inputs_e):
        gate_w, up_w, down_w, row_ids, row_weight = inputs_e
        exp_rows = input_ext[row_ids]
        exp_cot = (row_weight[:, None] * cot_ext[row_ids].astype(jnp.float32)).astype(jnp.bfloat16)
        gate_pre = jnp.dot(exp_rows, gate_w, preferred_element_type=jnp.float32)
        up_pre = jnp.dot(exp_rows, up_w, preferred_element_type=jnp.float32)
        sigmoid_g = jax.nn.sigmoid(gate_pre)
        activated = (gate_pre * sigmoid_g * up_pre).astype(jnp.bfloat16)
        grad_down = jnp.dot(activated.T, exp_cot, preferred_element_type=jnp.float32).astype(jnp.bfloat16)
        d_act = jnp.dot(exp_cot, down_w.T, preferred_element_type=jnp.float32)
        d_gate = (d_act * up_pre * sigmoid_g * (1.0 + gate_pre * (1.0 - sigmoid_g))).astype(jnp.bfloat16)
        d_up = (d_act * gate_pre * sigmoid_g).astype(jnp.bfloat16)
        grad_gate = jnp.dot(exp_rows.T, d_gate, preferred_element_type=jnp.float32).astype(jnp.bfloat16)
        grad_up = jnp.dot(exp_rows.T, d_up, preferred_element_type=jnp.float32).astype(jnp.bfloat16)
        returned = jnp.dot(d_gate, gate_w.T, preferred_element_type=jnp.float32)
        returned = returned + jnp.dot(d_up, up_w.T, preferred_element_type=jnp.float32)
        return (accum.at[row_ids].add(rounded(returned)), (grad_gate, grad_up, grad_down))
    accum, expert_out = lax.scan(expert_step, jnp.zeros((TOKENS + 1, D), jnp.float32), (gate_weights, up_weights, down_weights, slot_tok.reshape(EXPERTS, slot_count), slot_weight.reshape(EXPERTS, slot_count)))
    grad_gate, grad_up, grad_down = expert_out
    mixer_cot = (out_cot.astype(jnp.float32) + accum[:TOKENS]).astype(jnp.bfloat16)
    grad_proj = jnp.dot(mixer_cot.T, mixer_out, preferred_element_type=jnp.float32)
    head_rates = decay_rates(jnp.arange(HEADS).astype(jnp.float32), HEADS, TOKENS)
    positions = jnp.arange(TOKENS).astype(jnp.float32)
    head_cot = jnp.dot(mixer_cot, out_proj, preferred_element_type=jnp.float32).reshape(TOKENS, HEADS, DK)
    head_cot = (head_cot * position_norm(positions, head_rates)[:, :, None]).astype(jnp.bfloat16)
    grad_q, grad_k, grad_v = retention_grads(queries, keys, values, head_cot, entry_states, head_rates)
    return (grad_gate, grad_up, grad_down, grad_proj, grad_q, grad_k, grad_v)
```

```python
import jax
import jax.numpy as jnp
from jax import lax
from jax.experimental import pallas as pl
from jax.experimental.pallas import tpu as pltpu
from jax.sharding import Mesh
from jax.sharding import PartitionSpec as P

DK = 64
SPAN = 128
SP = ("sp_0", "sp_1", "sp_2")
MESH = pl.DeviceIdType.MESH
BF16 = jnp.bfloat16
F32 = jnp.float32

PLANES = 8
GROUP = 8
RING = 4
SLOTS = 8
ISSUE = "thin1 thin6 thin2 thin5 thin3 thin4 thin7 wide0 wide1 wide7".split()
WIDE = {0: (0, 1), 1: (0,), 7: (1,)}
WIDE_AT = [(k, kind) for k, kinds in WIDE.items() for kind in kinds]
THIN = {k: tuple(kind for kind in range(2) if kind not in WIDE.get(k, ())) for k in range(PLANES)}
BATCHES = ((6, 2, 5), (0, 3), (4, 1, 7))
AT = {k: i for i, k in enumerate(k for batch in BATCHES for k in batch)}
SCHEDULE = (
    "arrive1 arrive6 pass1 arrive2 pass6 arrive5 pass2 arrive3 pass5 mix1 arrive4 pass3 "
    "batch0 arrive7 pass4 batch1 second6 second2 second5 pass7 second0 second3 batch2 mix2 "
    "finish6 finish2 finish5 finish0 finish3 second4 second1 second7 mix3 finish4 finish1 "
    "finish7 grads0 grads1 grads2 grads3"
).split()
ROWS_TO_COLS = (((0,), (0,)), ((), ()))
COLS_TO_COLS = (((1,), (1,)), ((), ()))


def place():
    z, x, c = (lax.axis_index(axis) for axis in SP)
    return z, x * 2 + c, lax.axis_index("tp")


def device(z, member, ring):
    return (z, member // 2, member % 2, ring)


def send(src, dst, send_sem, recv_sem, target):
    copy = pltpu.make_async_remote_copy(
        src_ref=src,
        dst_ref=dst,
        send_sem=send_sem,
        recv_sem=recv_sem,
        device_id=target,
        device_id_type=MESH,
    )
    copy.start()


def wait_recv(ref, sem, me):
    pltpu.make_async_remote_copy(
        src_ref=ref, dst_ref=ref, send_sem=sem, recv_sem=sem, device_id=me, device_id_type=MESH
    ).wait_recv()


def wait_send(ref, sem, me):
    pltpu.make_async_remote_copy(
        src_ref=ref, dst_ref=ref, send_sem=sem, recv_sem=sem, device_id=me, device_id_type=MESH
    ).wait_send()


def block(index, size):
    return pl.ds(pl.multiple_of(index * size, size), size)


def loop(low, high, body):
    def step(i, carry):
        body(i)
        return carry

    lax.fori_loop(low, high, step, 0)


def moe_kernel(
    routes_ref,
    weights_ref,
    input_any,
    cot_any,
    mixer_any,
    gate_any,
    up_any,
    down_any,
    mixed_ref,
    mixers_ref,
    grad_gate_ref,
    grad_up_ref,
    grad_down_ref,
    tokens_in,
    cot_in,
    pick,
    slot_weight,
    sent,
    direct,
    full,
    gate_w,
    up_w,
    down_w,
    act,
    d_gate,
    d_up,
    part,
    raw,
    total,
    first,
    second,
    summed,
    returned,
    load_sem,
    sent_sem,
    wide_sem,
    got_sem,
    wide_got_sem,
    mix_send_sem,
    mix_recv_sem,
    ring_send_sem,
    ring_recv_sem,
    pass_send_sem,
    pass_recv_sem,
    raw_send_sem,
    raw_recv_sem,
    first_send_sem,
    first_recv_sem,
    second_send_sem,
    second_recv_sem,
    back_send_sem,
    back_recv_sem,
    cot_send_sem,
    cot_recv_sem,
    last_send_sem,
    last_recv_sem,
):
    z, m, y = place()
    s = z * GROUP + m
    above, below, across = (y + 1) % RING, (y + RING - 1) % RING, (y + 2) % RING
    me = device(z, m, y)
    ring = (device(z, m, above), device(z, m, below))
    experts = PLANES * GROUP
    tok_rows, wide = tokens_in.shape
    width = wide // RING
    rows = experts * SLOTS
    group_rows = GROUP * SLOTS

    barrier = pltpu.get_barrier_semaphore()

    def greet(d):
        other = (s + d) % experts
        pl.semaphore_signal(
            barrier,
            inc=1,
            device_id=device(other // GROUP, other % GROUP, y),
            device_id_type=MESH,
        )

    loop(1, experts, greet)
    for other in ring:
        pl.semaphore_signal(barrier, inc=1, device_id=other, device_id_type=MESH)

    own_mixer = mixers_ref.at[block(m, SPAN), :]
    loads = [
        pltpu.make_async_copy(src, dst, load_sem.at[i])
        for i, (src, dst) in enumerate(
            (
                (input_any, tokens_in),
                (cot_any, cot_in),
                (mixer_any, own_mixer),
                (gate_any, gate_w),
                (up_any, up_w),
                (down_any, down_w),
            )
        )
    ]
    for load in loads:
        load.start()

    own_cols = block(y, width)
    own_rows = block(s, SLOTS)
    with jax.named_scope("route"):
        chosen, weight = routes_ref[...], weights_ref[...]
        expert_ids = lax.broadcasted_iota(jnp.int32, (experts, tok_rows), 0)
        hits = [expert_ids == chosen[k : k + 1, :] for k in range(chosen.shape[0])]
        named = sum(jnp.where(hit, 1.0, 0.0) for hit in hits).astype(BF16)
        above_ids = lax.broadcasted_iota(jnp.int32, (tok_rows, tok_rows), 0)
        token_ids = lax.broadcasted_iota(jnp.int32, (tok_rows, tok_rows), 1)
        before = jnp.where(above_ids < token_ids, 1.0, 0.0).astype(BF16)
        earlier = jnp.dot(named, before, preferred_element_type=F32)
        slot_ids = lax.broadcasted_iota(jnp.int32, (rows, tok_rows), 0)
        picked, weighed = 0.0, 0.0
        for k, hit in enumerate(hits):
            slot = jnp.sum(jnp.where(hit, earlier, 0.0), axis=0, keepdims=True)
            taken = slot_ids == chosen[k : k + 1, :] * SLOTS + slot.astype(jnp.int32)
            picked = picked + jnp.where(taken, 1.0, 0.0)
            weighed = weighed + jnp.where(taken, weight[k : k + 1, :], 0.0)
        pick[...] = picked.astype(BF16)
        slot_weight[...] = jnp.sum(weighed, axis=1, keepdims=True)
    loads[0].wait()
    loads[1].wait()
    with jax.named_scope("prep"):
        sent[0] = jnp.dot(pick[...], tokens_in[:, own_cols], preferred_element_type=F32).astype(
            BF16
        )
        sent[1] = (
            slot_weight[...]
            * jnp.dot(pick[...], cot_in[:, own_cols], preferred_element_type=F32)
        ).astype(BF16)
        for i, (k, kind) in enumerate(WIDE_AT):
            there = block((z + k) % PLANES, group_rows)
            if kind == 0:
                line = jnp.dot(pick[there, :], tokens_in[...], preferred_element_type=F32)
            else:
                line = slot_weight[there, :] * jnp.dot(
                    pick[there, :], cot_in[...], preferred_element_type=F32
                )
            direct[i] = line.astype(BF16)
        for kind in range(2):
            full[kind, block(AT[0] * GROUP + m, SLOTS), :] = direct[
                WIDE_AT.index((0, kind)), block(m, SLOTS), :
            ]
    loads[2].wait()

    with jax.named_scope("meet"):
        pl.semaphore_wait(barrier, experts + 1)

    def thin_kinds(k):
        return (slice(None),) if len(THIN[k]) == 2 else THIN[k]

    for step in ISSUE:
        width_name, k = step[:-1], int(step[-1])
        to_z = (z + k) % PLANES
        land = block(AT[k] * GROUP + m, SLOTS)

        def dispatch(j, to_z=to_z, k=k, land=land, wide_turn=width_name == "wide"):
            to_m = (m + j) % GROUP
            target = device(to_z, to_m, y)
            for kind in WIDE.get(k, ()) if wide_turn else ():
                send(
                    direct.at[WIDE_AT.index((k, kind)), block(to_m, SLOTS), :],
                    full.at[kind, land, :],
                    wide_sem,
                    wide_got_sem.at[k],
                    target,
                )
            for kind in () if wide_turn else thin_kinds(k):
                send(
                    sent.at[kind, block(to_z * GROUP + to_m, SLOTS), :],
                    full.at[kind, land, own_cols],
                    sent_sem,
                    got_sem.at[k],
                    target,
                )

        loop(1 if k == 0 else 0, GROUP, dispatch)

    right_m, left_m, partner_m = (m + 2) % GROUP, (m + GROUP - 2) % GROUP, m + 1 - 2 * (m % 2)
    right, left, partner = (device(z, other, y) for other in (right_m, left_m, partner_m))
    half_span = SPAN // 2

    def share(ref, slot, target):
        send(ref, ref, mix_send_sem, mix_recv_sem.at[slot], target)

    def mix(stage):
        if stage == 0:
            for slot, target in enumerate((right, left, partner)):
                share(own_mixer, slot, target)
        if stage == 1:
            for slot, (owner, target) in enumerate(((left_m, right), (right_m, left))):
                wait_recv(own_mixer, mix_recv_sem.at[slot], me)
                share(mixers_ref.at[block(owner, SPAN), :], 5 + slot, partner)
                piece = mixers_ref.at[block(owner * 2 + slot, half_span), :]
                share(piece, 3 + slot, target)
        if stage == 2:
            for slot in range(2):
                wait_recv(mixers_ref.at[block(m * 2, half_span), :], mix_recv_sem.at[3 + slot], me)
            share(mixers_ref.at[block((m + 4) % GROUP, SPAN), :], 7, partner)
        if stage == 3:
            for slot in (2, 5, 6, 7):
                wait_recv(own_mixer, mix_recv_sem.at[slot], me)

    def take_rows(k):
        return pl.ds(AT[k] * group_rows, group_rows)

    def arrive(k):
        for kind in thin_kinds(k):
            piece = full.at[kind, take_rows(k), own_cols]
            wait_recv(piece, got_sem.at[k], me)
            for side in range(2):
                send(piece, piece, ring_send_sem, ring_recv_sem.at[side, k], ring[side])

    def half_of(k, side, cols):
        if len(THIN[k]) == 2:
            return full.at[side, take_rows(k), cols]
        start = AT[k] * group_rows + side * (group_rows // 2)
        return full.at[THIN[k][0], pl.ds(start, group_rows // 2), cols]

    def pass_on(k):
        for side, owner in enumerate((below, above)):
            for kind in thin_kinds(k):
                wait_recv(full.at[kind, take_rows(k), own_cols], ring_recv_sem.at[side, k], me)
            piece = half_of(k, side, block(owner, width))
            send(piece, piece, pass_send_sem, pass_recv_sem.at[side, k], ring[side])

    def complete(k):
        if THIN[k]:
            for side in range(2):
                wait_recv(half_of(k, side, own_cols), pass_recv_sem.at[side, k], me)
        if k in WIDE:
            arrived = group_rows - SLOTS if k == 0 else group_rows
            kinds = slice(None) if len(WIDE[k]) == 2 else WIDE[k][0]
            wait_recv(full.at[kinds, pl.ds(0, arrived), :], wide_got_sem.at[k], me)

    piece_cols = width // 2
    far = (across * 2, across * 2 + 1)
    near_raw = (above * 2 + 1, below * 2)
    near_sum = (above * 2, below * 2 + 1)

    def compute(batch):
        here = pl.ds(AT[batch[0]] * group_rows, len(batch) * group_rows)
        gate_pre = jnp.dot(full[0, here, :], gate_w[...], preferred_element_type=F32)
        up_pre = jnp.dot(full[0, here, :], up_w[...], preferred_element_type=F32)
        d_act = lax.dot_general(
            full[1, here, :], down_w[...], COLS_TO_COLS, preferred_element_type=F32
        )
        sigmoid_g = jax.nn.sigmoid(gate_pre)
        act[here, :] = (gate_pre * sigmoid_g * up_pre).astype(BF16)
        d_gate[here, :] = (
            d_act * up_pre * sigmoid_g * (1.0 + gate_pre * (1.0 - sigmoid_g))
        ).astype(BF16)
        d_up[here, :] = (d_act * gate_pre * sigmoid_g).astype(BF16)

        def backward(n):
            back_rows = block(n, piece_cols)
            back = lax.dot_general(
                d_gate[here, :], gate_w[back_rows, :], COLS_TO_COLS, preferred_element_type=F32
            )
            back = back + lax.dot_general(
                d_up[here, :], up_w[back_rows, :], COLS_TO_COLS, preferred_element_type=F32
            )
            part[n, here, :] = back.astype(BF16)

        loop(0, 2 * RING, backward)

    def send_parts(batch):
        for source, buffer, send_sem, recv_sem in (
            (far, raw, raw_send_sem, raw_recv_sem),
            (near_raw, first, first_send_sem, first_recv_sem),
        ):
            for k in batch:
                here = take_rows(k)
                for side in range(2):
                    send(
                        part.at[source[side], here, :],
                        buffer.at[side, here, :],
                        send_sem,
                        recv_sem.at[side, k],
                        ring[side],
                    )

    def send_second(k):
        here = take_rows(k)
        for side in range(2):
            wait_recv(raw.at[side, here, :], raw_recv_sem.at[side, k], me)
            total[side, here, :] = (
                raw[side, here, :].astype(F32) + part[near_sum[side], here, :].astype(F32)
            ).astype(BF16)
            send(
                total.at[side, here, :],
                second.at[side, here, :],
                second_send_sem,
                second_recv_sem.at[side, k],
                ring[side],
            )

    def finish(k):
        here = take_rows(k)
        to_z = (z + PLANES - k) % PLANES
        for side in range(2):
            wait_recv(first.at[side, here, :], first_recv_sem.at[side, k], me)
            wait_recv(second.at[side, here, :], second_recv_sem.at[side, k], me)
        for h in range(2):
            summed[here, pl.ds(h * piece_cols, piece_cols)] = (
                part[y * 2 + h, here, :].astype(F32)
                + first[1 - h, here, :].astype(F32)
                + second[h, here, :].astype(F32)
            ).astype(BF16)
        if k == 0:
            returned[own_rows, :] = summed[block(AT[0] * GROUP + m, SLOTS), :]

        def give_back(j):
            to_m = (m + j) % GROUP
            send(
                summed.at[block(AT[k] * GROUP + to_m, SLOTS), :],
                returned.at[own_rows, :],
                back_send_sem,
                back_recv_sem,
                device(to_z, to_m, y),
            )

        loop(1 if k == 0 else 0, GROUP, give_back)

    tile = wide // PLANES

    def weight_grads(i):
        here = pl.ds(i * tile, tile)
        tokens = full[0, :, here].T
        grad_gate_ref[here, :] = jnp.dot(
            tokens, d_gate[...], preferred_element_type=F32
        ).astype(BF16)
        grad_up_ref[here, :] = jnp.dot(tokens, d_up[...], preferred_element_type=F32).astype(BF16)
        grad_down_ref[:, here] = jnp.dot(
            act[...].T, full[1, :, here], preferred_element_type=F32
        ).astype(BF16)

    stages = dict(arrive=arrive, second=send_second, finish=finish, mix=mix)
    stages["pass"] = pass_on
    mix(0)
    for step in SCHEDULE:
        stage, k = step[:-1], int(step[-1])
        with jax.named_scope(step):
            if stage == "batch":
                if k == 0:
                    for load in loads[3:]:
                        load.wait()
                for member in BATCHES[k]:
                    complete(member)
                compute(BATCHES[k])
                send_parts(BATCHES[k])
            elif stage == "grads":
                weight_grads(2 * k)
                weight_grads(2 * k + 1)
            else:
                stages[stage](k)

    all_but_own = pl.ds(0, rows - SLOTS)
    with jax.named_scope("back"):
        wait_recv(returned.at[all_but_own, :], back_recv_sem, me)
    with jax.named_scope("combine"):
        mixed_ref[:, own_cols] = (
            cot_in[:, own_cols].astype(F32)
            + lax.dot_general(pick[...], returned[...], ROWS_TO_COLS, preferred_element_type=F32)
        ).astype(BF16)
    quarter = tok_rows // 4
    with jax.named_scope("cots"):
        for i in range(4):
            for side, n in enumerate((i, (i + 2) % 4)):
                piece = mixed_ref.at[pl.ds(n * quarter, quarter), own_cols]
                send(piece, piece, cot_send_sem, cot_recv_sem.at[side, n], ring[side])
        for i in range(4):
            for side, (owner, n) in enumerate(((below, i), (above, (i + 2) % 4))):
                piece = mixed_ref.at[pl.ds(n * quarter, quarter), block(owner, width)]
                wait_recv(piece, cot_recv_sem.at[side, n], me)
                if i < 2:
                    send(piece, piece, last_send_sem, last_recv_sem.at[side, i], ring[side])
        for i in range(2):
            for side in range(2):
                wait_recv(
                    mixed_ref.at[pl.ds(0, quarter), own_cols], last_recv_sem.at[side, i], me
                )

    thin_rows = sum(len(kinds) for kinds in THIN.values()) * group_rows // 2
    wide_rows = rows - thin_rows - SLOTS
    wait_send(sent.at[:, pl.ds(0, thin_rows), :], sent_sem, me)
    wait_send(full.at[:, pl.ds(0, wide_rows), :], wide_sem, me)
    wait_send(mixers_ref.at[pl.ds(0, (GROUP - 1) * SPAN), :], mix_send_sem, me)
    wait_send(full.at[:, pl.ds(0, thin_rows), pl.ds(0, 2 * width)], ring_send_sem, me)
    wait_send(full.at[:, pl.ds(0, thin_rows), own_cols], pass_send_sem, me)
    wait_send(raw, raw_send_sem, me)
    wait_send(first, first_send_sem, me)
    wait_send(second, second_send_sem, me)
    wait_send(returned.at[all_but_own, :], back_send_sem, me)
    wait_send(mixed_ref.at[:, pl.ds(0, 2 * width)], cot_send_sem, me)
    wait_send(mixed_ref.at[:, own_cols], last_send_sem, me)


def moe(routes, route_weights, layer_input, out_cot, mixer_out, gate_w, up_w, down_w):
    tokens, wide = layer_input.shape
    rows, hidden = PLANES * GROUP * SLOTS, gate_w.shape[1]
    width = wide // RING
    vmem = pl.BlockSpec(memory_space=pltpu.VMEM)
    dma, many = pltpu.SemaphoreType.DMA, pltpu.SemaphoreType.DMA((2, PLANES))
    return pl.pallas_call(
        moe_kernel,
        out_shape=(
            jax.ShapeDtypeStruct((tokens, wide), BF16),
            jax.ShapeDtypeStruct((GROUP * tokens, width), BF16),
            jax.ShapeDtypeStruct((wide, hidden), BF16),
            jax.ShapeDtypeStruct((wide, hidden), BF16),
            jax.ShapeDtypeStruct((hidden, wide), BF16),
        ),
        in_specs=[vmem] * 2 + [pl.BlockSpec(memory_space=pl.ANY)] * 6,
        out_specs=(vmem,) * 5,
        scratch_shapes=[
            pltpu.VMEM((tokens, wide), BF16),
            pltpu.VMEM((tokens, wide), BF16),
            pltpu.VMEM((rows, tokens), BF16),
            pltpu.VMEM((rows, 1), F32),
            pltpu.VMEM((2, rows, width), BF16),
            pltpu.VMEM((len(WIDE_AT), GROUP * SLOTS, wide), BF16),
            pltpu.VMEM((2, rows, wide), BF16),
            pltpu.VMEM((wide, hidden), BF16),
            pltpu.VMEM((wide, hidden), BF16),
            pltpu.VMEM((hidden, wide), BF16),
            pltpu.VMEM((rows, hidden), BF16),
            pltpu.VMEM((rows, hidden), BF16),
            pltpu.VMEM((rows, hidden), BF16),
            pltpu.VMEM((2 * RING, rows, width // 2), BF16),
            pltpu.VMEM((2, rows, width // 2), BF16),
            pltpu.VMEM((2, rows, width // 2), BF16),
            pltpu.VMEM((2, rows, width // 2), BF16),
            pltpu.VMEM((2, rows, width // 2), BF16),
            pltpu.VMEM((rows, width), BF16),
            pltpu.VMEM((rows, width), BF16),
            dma((6,)),
            dma,
            dma,
            dma((PLANES,)),
            dma((PLANES,)),
            dma,
            dma((8,)),
            dma,
            many,
            dma,
            many,
            dma,
            many,
            dma,
            many,
            dma,
            many,
            dma,
            dma,
            dma,
            dma((2, 4)),
            dma,
            dma((2, 2)),
        ],
        compiler_params=pltpu.CompilerParams(
            collective_id=0, has_side_effects=True, vmem_limit_bytes=56 * 1024 * 1024
        ),
        name="moe",
    )(routes, route_weights, layer_input, out_cot, mixer_out, gate_w, up_w, down_w)


def tail_kernel(
    power_ref,
    mixed_ref,
    mixers_ref,
    backs_ref,
    state_ref,
    proj_ref,
    turned,
    gathered,
    heads,
    inside,
    sum_out,
    sums,
    answers,
    pieces,
    shares,
    head_send_sem,
    head_recv_sem,
    turn_send_sem,
    turn_recv_sem,
    sum_send_sem,
    sum_recv_sem,
    share_send_sem,
    share_recv_sem,
    state_send_sem,
    state_recv_sem,
):
    z, m, y = place()
    me = device(z, m, y)
    barrier = pltpu.get_barrier_semaphore()

    def greet(j):
        for other in (device(z, (m + j) % GROUP, y), device((z + j) % PLANES, m, y)):
            pl.semaphore_signal(barrier, inc=1, device_id=other, device_id_type=MESH)

    loop(1, GROUP, greet)
    slab = mixed_ref.shape[1] // PLANES // GROUP
    per = SPAN // slab
    for n in range(mixed_ref.shape[1] // SPAN):
        spun = mixed_ref[:, pl.ds(n * SPAN, SPAN)].T
        first = n * per
        turned[first // GROUP, pl.ds(first % GROUP, per)] = spun.reshape(per, slab, SPAN)
    gathered[:, :, block(m, SPAN)] = turned[:, m]
    heads[m] = backs_ref[m]
    pl.semaphore_wait(barrier, GROUP + PLANES - 2)

    def send_head(j):
        to_m = (m + j) % GROUP
        send(backs_ref.at[to_m], heads.at[m], head_send_sem, head_recv_sem, device(z, to_m, y))

    def send_turned(j):
        to_m = (m + j) % GROUP
        send(
            turned.at[:, to_m],
            gathered.at[:, :, block(m, SPAN)],
            turn_send_sem,
            turn_recv_sem,
            device(z, to_m, y),
        )

    loop(1, GROUP, send_head)
    loop(1, GROUP, send_turned)
    others = pl.ds(0, GROUP - 1)
    wait_recv(heads.at[others], head_recv_sem, me)
    running = jnp.zeros(heads.shape[1:], F32)
    for i in reversed(range(GROUP)):
        inside[i] = running
        running = heads[i].astype(F32) + power_ref[1] * running
    sum_out[...] = running.astype(BF16)
    sums[z] = sum_out[...]

    def send_sum(j):
        send(sum_out, sums.at[z], sum_send_sem, sum_recv_sem, device((z + j) % PLANES, m, y))

    loop(1, PLANES, send_sum)

    wait_recv(gathered.at[:, :, pl.ds(0, (GROUP - 1) * SPAN)], turn_recv_sem, me)
    product = jnp.dot(
        gathered[...].reshape(PLANES * slab, GROUP * SPAN),
        mixers_ref[...],
        preferred_element_type=F32,
    )
    pieces[...] = product.astype(BF16).reshape(pieces.shape)
    shares[z] = pieces[z]

    def send_share(j):
        to_z = (z + j) % PLANES
        send(pieces.at[to_z], shares.at[z], share_send_sem, share_recv_sem, device(to_z, m, y))

    loop(1, PLANES, send_share)

    wait_recv(sums.at[others], sum_recv_sem, me)
    later = jnp.zeros(heads.shape[1:], F32)
    for i in range(PLANES):
        later = later + power_ref[GROUP + i] * sums[i].astype(F32)
    for i in range(GROUP):
        answers[i] = (inside[i] + power_ref[GROUP - 1 - i] * later).astype(BF16)
    state_ref[m] = answers[m]

    def send_state(j):
        to_m = (m + j) % GROUP
        send(
            answers.at[to_m], state_ref.at[m], state_send_sem, state_recv_sem, device(z, to_m, y)
        )

    loop(1, GROUP, send_state)

    wait_recv(shares.at[others], share_recv_sem, me)
    proj = shares[0].astype(F32)
    for i in range(1, PLANES):
        proj = proj + shares[i].astype(F32)
    proj_ref[...] = proj
    wait_recv(state_ref.at[others], state_recv_sem, me)

    wait_send(heads.at[others], head_send_sem, me)
    wait_send(gathered.at[:, :, pl.ds(0, (GROUP - 1) * SPAN)], turn_send_sem, me)
    wait_send(sums.at[others], sum_send_sem, me)
    wait_send(shares.at[others], share_send_sem, me)
    wait_send(answers.at[others], state_send_sem, me)


def tail(powers, mixed, mixers, backs):
    wide, width = mixed.shape[1], mixers.shape[1]
    slab = wide // PLANES // GROUP
    state = backs.shape[1:]
    vmem = pl.BlockSpec(memory_space=pltpu.VMEM)
    return pl.pallas_call(
        tail_kernel,
        out_shape=(
            jax.ShapeDtypeStruct(backs.shape, BF16),
            jax.ShapeDtypeStruct((slab, width), F32),
        ),
        in_specs=[pl.BlockSpec(memory_space=pltpu.SMEM)] + [vmem] * 3,
        out_specs=(vmem,) * 2,
        scratch_shapes=[
            pltpu.VMEM((PLANES, GROUP, slab, SPAN), BF16),
            pltpu.VMEM((PLANES, slab, GROUP * SPAN), BF16),
            pltpu.VMEM((GROUP, *state), BF16),
            pltpu.VMEM((GROUP, *state), F32),
            pltpu.VMEM(state, BF16),
            pltpu.VMEM((PLANES, *state), BF16),
            pltpu.VMEM((GROUP, *state), BF16),
            pltpu.VMEM((PLANES, slab, width), BF16),
            pltpu.VMEM((PLANES, slab, width), BF16),
        ]
        + [pltpu.SemaphoreType.DMA] * 10,
        compiler_params=pltpu.CompilerParams(
            collective_id=1, has_side_effects=True, vmem_limit_bytes=32 * 1024 * 1024
        ),
        name="tail",
    )(powers, mixed, mixers, backs)


def decay_rates(head_ids, head_count, token_count):
    half_count = head_count // 2
    fraction = jnp.minimum(head_ids, half_count) / half_count
    base_rate = jnp.exp(
        (1.0 - fraction) * jnp.log(1.0 / 32.0) + fraction * jnp.log(1.0 / token_count)
    )
    return base_rate * (1.0 + jnp.maximum(head_ids - half_count, 0.0) / half_count)


def position_norm(positions, head_rates):
    return jnp.sqrt(
        jnp.expm1(-2.0 * head_rates)[None, :]
        / jnp.expm1(-2.0 * head_rates[None, :] * (positions[:, None] + 1.0))
    )


def per_device(
    layer_input,
    out_cot,
    routes,
    route_weights,
    gate_weights,
    up_weights,
    down_weights,
    out_proj,
    queries,
    keys,
    values,
    mixer_out,
    entry_states,
):
    tok_rows, model_width = layer_input.shape
    experts = lax.axis_size(SP)
    narrow = lax.axis_size("tp")
    mixer_cot, mixers, grad_gate, grad_up, grad_down = moe(
        routes.T,
        route_weights.T,
        layer_input,
        out_cot,
        mixer_out,
        gate_weights[0],
        up_weights[0],
        down_weights[0],
    )
    head_count = queries.shape[1] // DK
    head_ids = (lax.axis_index("tp") * head_count + jnp.arange(head_count, dtype=jnp.int32)).astype(
        jnp.float32
    )
    head_rates = decay_rates(head_ids, head_count * narrow, tok_rows * experts)
    positions = (lax.axis_index(SP) * tok_rows + jnp.arange(tok_rows, dtype=jnp.int32)).astype(
        jnp.float32
    )
    head_cot = jnp.dot(mixer_cot, out_proj, preferred_element_type=jnp.float32).reshape(
        tok_rows, head_count, DK
    )
    head_cot = (head_cot * position_norm(positions, head_rates)[:, :, None]).astype(jnp.bfloat16)
    span_count = tok_rows // SPAN
    span_shape = (span_count, SPAN, head_count, DK)
    span_query = queries.reshape(span_shape)
    span_key = keys.reshape(span_shape)
    span_value = values.reshape(span_shape)
    span_cot = head_cot.reshape(span_shape)
    key_scale = DK ** (-0.5)
    offsets = jnp.arange(SPAN, dtype=jnp.float32)
    distance = offsets[:, None] - offsets[None, :]
    decay_mat = jnp.where(
        distance[None] >= 0,
        jnp.exp(-head_rates[:, None, None] * jnp.maximum(distance, 0.0)[None]),
        0.0,
    )
    fwd_weights = (
        jnp.einsum("cihd,cjhd->chij", span_query, span_key, preferred_element_type=jnp.float32)
        * key_scale
        * decay_mat[None]
    ).astype(jnp.bfloat16)
    back_weights = (
        jnp.einsum("cihd,cjhd->chij", span_cot, span_value, preferred_element_type=jnp.float32)
        * decay_mat[None]
    ).astype(jnp.bfloat16)
    tail_decay = jnp.exp(-head_rates[None, :] * (SPAN - 1.0 - offsets)[:, None])
    lead_decay = jnp.exp(-head_rates[None, :] * (offsets + 1.0)[:, None])
    query_wide = span_query.astype(jnp.float32)
    key_wide = span_key.astype(jnp.float32)
    value_wide = span_value.astype(jnp.float32)
    cot_wide = span_cot.astype(jnp.float32)
    backs = jnp.einsum(
        "cihd,cihe->chde",
        query_wide * lead_decay[None, :, :, None],
        cot_wide,
        precision=lax.Precision.HIGHEST,
    )
    member = lax.axis_index(SP[1:])
    span_log = -SPAN * lax.dynamic_index_in_dim(head_rates, member, 0, keepdims=False)
    steps = jnp.arange(GROUP, dtype=F32)
    apart = steps - lax.axis_index(SP[0]).astype(F32) - 1.0
    powers = jnp.concatenate(
        [
            jnp.exp(span_log * steps),
            jnp.where(apart >= 0, jnp.exp(GROUP * span_log * jnp.maximum(apart, 0.0)), 0.0),
        ]
    )
    flat_state = (head_count, DK * DK // SPAN, SPAN)
    states, grad_proj = tail(powers, mixer_cot, mixers, backs[0].reshape(flat_state).astype(BF16))
    rev_states = states.reshape(1, head_count, DK, DK).astype(F32)
    fwd_stack = entry_states
    grad_q = key_scale * jnp.einsum(
        "chij,cjhd->cihd", back_weights, span_key, preferred_element_type=jnp.float32
    )
    grad_q = grad_q + lead_decay[None, :, :, None] * jnp.einsum(
        "chde,cihe->cihd", fwd_stack, cot_wide, precision=lax.Precision.HIGHEST
    )
    grad_k = jnp.einsum(
        "chij,cihd->cjhd", back_weights, span_query, preferred_element_type=jnp.float32
    )
    grad_k = key_scale * (
        grad_k
        + tail_decay[None, :, :, None]
        * jnp.einsum("chde,cjhe->cjhd", rev_states, value_wide, precision=lax.Precision.HIGHEST)
    )
    grad_v = jnp.einsum(
        "chij,cihe->cjhe", fwd_weights, span_cot, preferred_element_type=jnp.float32
    )
    grad_v = grad_v + key_scale * tail_decay[None, :, :, None] * jnp.einsum(
        "chde,cjhd->cjhe", rev_states, key_wide, precision=lax.Precision.HIGHEST
    )
    flat_shape = (tok_rows, head_count * DK)
    return (
        grad_gate[None],
        grad_up[None],
        grad_down[None],
        grad_proj,
        grad_q.reshape(flat_shape).astype(jnp.bfloat16),
        grad_k.reshape(flat_shape).astype(jnp.bfloat16),
        grad_v.reshape(flat_shape).astype(jnp.bfloat16),
    )


def solution(mesh):
    torus = Mesh(mesh.devices.reshape(8, 4, 2, mesh.shape["tp"]), ("sp_0", "sp_1", "sp_2", "tp"))
    return jax.shard_map(
        per_device,
        mesh=torus,
        in_specs=(
            P(SP, None),
            P(SP, None),
            P(SP, None),
            P(SP, None),
            P(SP, None, "tp"),
            P(SP, None, "tp"),
            P(SP, "tp", None),
            P(None, "tp"),
            P(SP, "tp"),
            P(SP, "tp"),
            P(SP, "tp"),
            P(SP, "tp"),
            P(SP, "tp", None, None),
        ),
        out_specs=(
            P(SP, None, "tp"),
            P(SP, None, "tp"),
            P(SP, "tp", None),
            P(SP, "tp"),
            P(SP, "tp"),
            P(SP, "tp"),
            P(SP, "tp"),
        ),
        check_vma=False,
    )
```
